32 devices in a mesh: dp: 4 (over y, x), kv: 4 (over z), tp: 2 (over core).
Axes of the slice: x: 2, y: 2, z: 4, core: 2. Of those that a mesh axis runs over, the one named last changes fastest.
Arguments:
- tokens: bfloat16 [24, 4096], P('dp', 'kv'), may hold values from -64 to 64
- lengths: int32 [24], P('dp'), may hold values from 128 to 1024, as said below
- attn_gain: float32 [4096], P('kv'), may hold values from 0.1 to 1.9
- query_weight: bfloat16 [4096, 4096], P('kv', 'tp'), may hold values from -0.09375 to 0.09375
- key_weight: bfloat16 [4096, 256], P('kv', 'tp'), may hold values from -0.1875 to 0.1875
- value_weight: bfloat16 [4096, 256], P('kv', 'tp'), may hold values from -0.09375 to 0.09375
- forget_weight: bfloat16 [4096, 4], replicated, may hold values from -0.25 to 0.25
- forget_offset: float32 [4], P('tp'), may hold values from -6 to 0
- cache_keys: bfloat16 [24, 1024, 256], P('dp', 'kv', 'tp'), may hold values from -1600 to 1600
- cache_values: bfloat16 [24, 1024, 256], P('dp', 'kv', 'tp'), may hold values from -6 to 6
- gate_sum: float32 [24, 4, 1024], P('dp', 'tp', 'kv'), may hold values from -82 to 0
- out_weight: bfloat16 [4096, 4096], P('tp', 'kv'), may hold values from -0.1875 to 0.1875
- mlp_gain: float32 [4096], replicated, may hold values from 0.1 to 1.9
- up_weight: bfloat16 [4096, 16384], P(None, ('kv', 'tp')), may hold values from -0.09375 to 0.09375
- down_weight: bfloat16 [16384, 4096], P(('kv', 'tp')), may hold values from -0.0625 to 0.0625
Outputs:
- mixed: bfloat16 [24, 4096], P('dp', ('kv', 'tp'))
The draws below stay inside these ranges and needn't reach their ends.
Inputs may be any that keep to these rules, and one draw needn't show every extreme that they name: `lengths`: in every draw some sequence has all 1024 positions cached.
All inputs are finite; a program needn't handle non-finite values.
Results may differ from the reference program's by a relative error of at most 0.023.
Values may be sent and summed in bfloat16 or wider, within the bound.
A program may use at most 128 MiB of HBM per device.

```python
import math
import jax
import jax.numpy as jnp
from jax import lax

D = 4096
HEADS = 64
HD = 64
KEY_VALUE_HEADS = 4
FF = 16384
CTX_DEV = 256
SEQUENCE_COUNT = 24
CTX = 1024
HEAD_GROUPS = 2


def seq_lengths(key):
    shorter = jax.random.randint(jax.random.fold_in(key, 11), (SEQUENCE_COUNT,), CTX // 8, CTX // 2 + 1)
    longer = jax.random.randint(jax.random.fold_in(key, 12), (SEQUENCE_COUNT,), CTX // 2, CTX + 1)
    shuffled = jax.random.permutation(jax.random.fold_in(key, 13), SEQUENCE_COUNT)
    ranking = jnp.argsort(shuffled)
    chosen = jnp.where(ranking < max(SEQUENCE_COUNT // 4, 1), longer, shorter)
    return jnp.where(ranking == 0, CTX, chosen).astype(jnp.int32)


def draw_lengths(key, part):
    return seq_lengths(key)


def draw_tokens(key, part):
    columns = jnp.arange(D, dtype=jnp.float32) / D - 0.5
    normal_draw = jnp.clip(jax.random.normal(jax.random.fold_in(key, 41), (SEQUENCE_COUNT, D), jnp.float32), -6.0, 6.0)
    column_scale = jnp.exp(math.log(10.0) * columns)
    row_factor = jnp.exp(jax.random.uniform(jax.random.fold_in(key, 42), (SEQUENCE_COUNT, 1), jnp.float32, -0.5 * math.log(10.0), 0.5 * math.log(10.0)))
    return (normal_draw * column_scale[None, :] * row_factor).astype(jnp.bfloat16)


def draw_gate_sum(key, part):
    lengths = seq_lengths(key)
    live_span = lengths.astype(jnp.float32)[:, None, None]
    token_offsets = jnp.arange(CTX)
    shuffled = jax.random.permutation(jax.random.fold_in(key, 21), KEY_VALUE_HEADS)
    slow_heads = (shuffled < KEY_VALUE_HEADS // 2)[None, :, None]
    blocks = CTX // CTX_DEV
    block_factor = jnp.exp(jax.random.uniform(jax.random.fold_in(key, 22), (SEQUENCE_COUNT, KEY_VALUE_HEADS, blocks), jnp.float32, -math.log(2.0), math.log(2.0)))
    block_factor = jnp.repeat(block_factor, CTX_DEV, axis=2)
    data_factor = jax.random.uniform(jax.random.fold_in(key, 23), (SEQUENCE_COUNT, KEY_VALUE_HEADS, CTX), jnp.float32, 0.5, 1.5)
    falloff_speeds = jnp.where(slow_heads, 0.5 / live_span, 1.0 / 40.0) * block_factor * data_factor
    spike_locations = jax.random.randint(jax.random.fold_in(key, 24), (SEQUENCE_COUNT, KEY_VALUE_HEADS, 3), 0, lengths[:, None, None])
    spike_penalty = jnp.log(1.0 - jax.random.uniform(jax.random.fold_in(key, 25), (SEQUENCE_COUNT, KEY_VALUE_HEADS, 3), jnp.float32, 0.2, 0.45))
    spike_events = jnp.sum(jnp.where(token_offsets[None, None, None, :] == spike_locations[..., None], spike_penalty[..., None], 0.0), axis=2)
    active_mask = token_offsets[None, None, :] < lengths[:, None, None]
    gate_logarithms = jnp.where(active_mask, spike_events - falloff_speeds, 0.0)
    return (jnp.sum(gate_logarithms, axis=2, keepdims=True) - jnp.cumsum(gate_logarithms, axis=2)).astype(jnp.float32)


def draw_cache_keys(key, part):
    drawn = 2.0 * jnp.clip(jax.random.normal(jax.random.fold_in(key, 31), (SEQUENCE_COUNT, CTX, KEY_VALUE_HEADS, HD), jnp.float32), -6.0, 6.0)
    return drawn.reshape(SEQUENCE_COUNT, CTX, KEY_VALUE_HEADS * HD).astype(jnp.bfloat16)


def spiked(result, rng, source, target, parts, factor):
    def block_of(dim):
        return (jnp.arange(result.shape[dim]) // (result.shape[dim] // parts)).reshape((-1,) + (1,) * (result.ndim - 1 - dim))

    one_side = jax.random.permutation(rng, parts)[block_of(target)]
    other_side = (block_of(target) + parts // 2) % parts
    return jnp.where((block_of(source) == one_side) | (block_of(source) == other_side), factor * result, result)


def steps_of(key, extent, cuts, low, high):
    def one(position, blocks):
        steps = jax.random.uniform(jax.random.fold_in(jax.random.fold_in(key, 6), position), (blocks,), jnp.float32, low / len(cuts), high / len(cuts))
        return jnp.repeat(jnp.exp(steps), extent[position] // blocks).reshape((-1,) + (1,) * (len(extent) - position - 1))

    level = one(*cuts[0])
    for cut in cuts[1:]:
        level = level * one(*cut)
    return level


def normal_values(key, shape, width, bound, cuts=(), held_as=jnp.bfloat16):
    values = width * jax.random.normal(key, shape, jnp.float32)
    if cuts:
        values = values * steps_of(key, shape, cuts, -0.22, 0.18)
    return jnp.clip(values, -bound, bound).astype(held_as)


def heavy_noise(rng, dims, deviation, reach, shards, heavy, kind=jnp.bfloat16):
    values = deviation * jax.random.normal(rng, dims, jnp.float32)
    if shards:
        values = values * steps_of(rng, dims, shards, -0.22, 0.18)
    return jnp.clip(spiked(values, jax.random.fold_in(rng, 3), *heavy), -reach, reach).astype(kind)


def setup_inputs(seed: int = 0) -> dict:
    arg_keys = jax.random.split(jax.random.key(seed), 16)
    return {
        "tokens": draw_tokens(jax.random.fold_in(arg_keys[15], 71), 0),
        "lengths": draw_lengths(jax.random.fold_in(arg_keys[15], 71), 0),
        "attn_gain": jnp.clip(1.0 + 0.18 * jax.random.normal(arg_keys[2], (D,), jnp.float32), 0.1, 1.9),
        "query_weight": normal_values(arg_keys[3], (D, HEADS * HD), D ** -0.5, 0.09375, ((0, 4), (1, 2))),
        "key_weight": normal_values(arg_keys[4], (D, KEY_VALUE_HEADS * HD), (D // 4) ** -0.5, 0.1875, ((0, 4), (1, 2))),
        "value_weight": normal_values(arg_keys[5], (D, KEY_VALUE_HEADS * HD), D ** -0.5, 0.09375, ((0, 4), (1, 2))),
        "forget_weight": normal_values(arg_keys[6], (D, KEY_VALUE_HEADS), (D // 8) ** -0.5, 0.25),
        "forget_offset": jnp.clip(-6.0 + 6.0 * jax.random.uniform(arg_keys[7], (KEY_VALUE_HEADS,), jnp.float32) ** steps_of(arg_keys[7], (KEY_VALUE_HEADS,), ((0, 2),), -0.2, 0.2), -6.0, 0.0),
        "cache_keys": draw_cache_keys(jax.random.fold_in(arg_keys[15], 71), 0),
        "cache_values": normal_values(arg_keys[9], (SEQUENCE_COUNT, CTX, KEY_VALUE_HEADS * HD), 1.0, 6.0, ((0, 4), (1, 4), (2, 2))),
        "gate_sum": draw_gate_sum(jax.random.fold_in(arg_keys[15], 71), 0),
        "out_weight": normal_values(arg_keys[11], (HEADS * HD, D), (D // 4) ** -0.5, 0.1875, ((0, 2), (1, 4))),
        "mlp_gain": jnp.clip(1.0 + 0.18 * jax.random.normal(arg_keys[12], (D,), jnp.float32), 0.1, 1.9),
        "up_weight": normal_values(arg_keys[13], (D, FF), D ** -0.5, 0.09375, ((1, 8),)),
        "down_weight": heavy_noise(arg_keys[14], (FF, D), FF ** -0.5, 0.0625, ((0, 8),), (0, 1, 8, 2.0)),
    }


epsilon = 1e-06

def reference(tokens, lengths, attn_gain, query_weight, key_weight, value_weight, forget_weight, forget_offset, cache_keys, cache_values, gate_sum, out_weight, mlp_gain, up_weight, down_weight):
    token_rows = tokens.astype(jnp.float32)
    row_scale = lax.rsqrt(lax.optimization_barrier(jnp.mean(token_rows * token_rows, axis=1, keepdims=True)) + epsilon)
    scaled_rows = (token_rows * attn_gain[None, :]).astype(jnp.bfloat16)
    queries = (jnp.dot(scaled_rows, query_weight, preferred_element_type=jnp.float32) * row_scale).astype(jnp.bfloat16)
    new_key = (jnp.dot(scaled_rows, key_weight, preferred_element_type=jnp.float32) * row_scale).astype(jnp.bfloat16)
    new_value = (jnp.dot(scaled_rows, value_weight, preferred_element_type=jnp.float32) * row_scale).astype(jnp.bfloat16)
    log_forget = jax.nn.log_sigmoid(jnp.dot(scaled_rows, forget_weight, preferred_element_type=jnp.float32) * row_scale + forget_offset[None, :])
    group_size = HEADS // KEY_VALUE_HEADS
    score_scale = HD ** (-0.5)
    token_offsets = jnp.arange(CTX)

    def one_sequence(inputs_one):
        query_row, key_rows, value_rows, gates, length, forget_row, own_key, own_value = inputs_one
        query_heads = query_row.astype(jnp.float32).reshape(KEY_VALUE_HEADS, group_size, HD)
        key_heads = key_rows.astype(jnp.float32).reshape(CTX, KEY_VALUE_HEADS, HD)
        value_heads = value_rows.astype(jnp.float32).reshape(CTX, KEY_VALUE_HEADS, HD)
        scores = jnp.einsum('kgd,pkd->kgp', query_heads, key_heads) * score_scale
        scores = scores + gates[:, None, :] + forget_row[:, None, None]
        active_mask = token_offsets < length
        scores = jnp.where(active_mask[None, None, :], scores, -jnp.inf)
        own_score = jnp.einsum('kgd,kd->kg', query_heads, own_key.astype(jnp.float32).reshape(KEY_VALUE_HEADS, HD)) * score_scale
        row_top = jnp.maximum(lax.optimization_barrier(jnp.max(scores, axis=2)), own_score)
        weight = jnp.exp(scores - row_top[..., None])
        own_weight = jnp.exp(own_score - row_top)
        totals = lax.optimization_barrier(jnp.sum(weight, axis=2)) + own_weight
        rounded = lax.optimization_barrier(weight.astype(jnp.bfloat16)).astype(jnp.float32)
        own_rounded = lax.optimization_barrier(own_weight.astype(jnp.bfloat16)).astype(jnp.float32)
        summed = jnp.einsum('kgp,pkd->kgd', rounded, value_heads)
        summed = summed + own_rounded[..., None] * own_value.astype(jnp.float32).reshape(KEY_VALUE_HEADS, 1, HD)
        return (summed / totals[..., None]).reshape(HEADS * HD).astype(jnp.bfloat16)
    attended = lax.map(one_sequence, (queries, cache_keys, cache_values, gate_sum, lengths, log_forget, new_key, new_value))
    group_width = HEADS * HD // HEAD_GROUPS
    summed_mid = token_rows
    for group_index in range(HEAD_GROUPS):
        partial_value = jnp.dot(attended[:, group_index * group_width:(group_index + 1) * group_width], out_weight[group_index * group_width:(group_index + 1) * group_width], preferred_element_type=jnp.float32)
        partial_value = lax.optimization_barrier(partial_value.astype(jnp.bfloat16)).astype(jnp.float32)
        summed_mid = summed_mid + partial_value
    mid_rows = summed_mid.astype(jnp.bfloat16)
    mid_wide = mid_rows.astype(jnp.float32)
    normed_mid = (mid_wide * mlp_gain[None, :] * lax.rsqrt(lax.optimization_barrier(jnp.mean(mid_wide * mid_wide, axis=1, keepdims=True)) + epsilon)).astype(jnp.bfloat16)
    hidden = jnp.square(jax.nn.relu(jnp.dot(normed_mid, up_weight, preferred_element_type=jnp.float32))).astype(jnp.bfloat16)
    return (mid_wide + jnp.dot(hidden, down_weight, preferred_element_type=jnp.float32)).astype(jnp.bfloat16)
```

```python
import functools

import jax
import jax.numpy as jnp
from jax import lax
from jax.experimental import pallas as pl
from jax.experimental.pallas import tpu as pltpu
from jax.sharding import PartitionSpec as P

D = 4096
HEADS = 64
HD = 64
KEY_VALUE_HEADS = 4


epsilon = 1e-06
floor_score = -1e30


def combined_all(x, axis, combine):
    everything = jax.tree.map(
        lambda part, kind: lax.all_gather(part.astype(kind), axis),
        x,
        (jnp.bfloat16, jnp.bfloat16, jnp.bfloat16),
    )

    def take(k):
        return jax.tree.map(lambda part, own: part[k].astype(own.dtype), everything, x)

    return lax.fori_loop(
        1, lax.axis_size(axis), lambda k, so_far: combine(so_far, take(k)), take(0)
    )


def combine_parts(earlier, later):
    first_top, first_total, first_values = earlier
    second_top, second_total, second_values = later
    merged_top = jnp.maximum(first_top, second_top)
    first_scale = jnp.exp(first_top - merged_top)
    second_scale = jnp.exp(second_top - merged_top)
    first_wide = jnp.repeat(first_scale, HD, axis=1)
    second_wide = jnp.repeat(second_scale, HD, axis=1)
    return (
        merged_top,
        first_total * first_scale + second_total * second_scale,
        first_values * first_wide + second_values * second_wide,
    )


def general_shards(
    tokens,
    lengths,
    attn_gain,
    query_weight,
    key_weight,
    value_weight,
    forget_weight,
    forget_offset,
    cache_keys,
    cache_values,
    gate_sum,
    out_weight,
    mlp_gain,
    up_weight,
    down_weight,
):
    row_count = tokens.shape[0]
    feature_cols = tokens.shape[1]
    kv_place = lax.axis_index("kv")
    tp_place = lax.axis_index("tp")
    local_heads = key_weight.shape[1] // HD
    group_size = HEADS // KEY_VALUE_HEADS
    token_rows = tokens.astype(jnp.float32)
    scaled_rows = (token_rows * attn_gain[None, :]).astype(jnp.bfloat16)
    square_part = jnp.sum(token_rows * token_rows, axis=1)
    query_part = jnp.dot(scaled_rows, query_weight, preferred_element_type=jnp.float32)
    key_part = jnp.dot(scaled_rows, key_weight, preferred_element_type=jnp.float32)
    value_part = jnp.dot(scaled_rows, value_weight, preferred_element_type=jnp.float32)
    gate_rows = lax.dynamic_slice(
        forget_weight,
        (kv_place * feature_cols, tp_place * local_heads),
        (feature_cols, local_heads),
    )
    forget_part = jnp.dot(scaled_rows, gate_rows, preferred_element_type=jnp.float32)
    query_sum, key_sum, value_sum, forget_sum, square_sum = lax.psum(
        (query_part, key_part, value_part, forget_part, square_part), "kv"
    )
    row_scale = lax.rsqrt(square_sum / D + epsilon)[:, None]
    queries = (query_sum * row_scale).astype(jnp.bfloat16)
    new_key = (key_sum * row_scale).astype(jnp.bfloat16)
    new_value = (value_sum * row_scale).astype(jnp.bfloat16)
    log_forget = jax.nn.log_sigmoid(forget_sum * row_scale + forget_offset[None, :])
    positions_here = cache_keys.shape[1]
    key_heads = cache_keys.reshape(row_count, positions_here, local_heads, HD)
    value_heads = cache_values.reshape(row_count, positions_here, local_heads, HD)
    query_heads = queries.reshape(row_count, local_heads, group_size, HD)
    scores = jnp.einsum(
        "skgd,spkd->skgp", query_heads, key_heads, preferred_element_type=jnp.float32
    ) * HD ** (-0.5)
    scores = scores + gate_sum[:, :, None, :] + log_forget[:, :, None, None]
    cache_pos = kv_place * positions_here + jnp.arange(positions_here)
    active_mask = (cache_pos[None, :] < lengths[:, None])[:, None, None, :]
    local_top = jnp.max(jnp.where(active_mask, scores, floor_score), axis=3)
    weights = jnp.where(active_mask, jnp.exp(scores - local_top[..., None]), 0.0)
    local_total = jnp.sum(weights, axis=3)
    local_values = jnp.einsum(
        "skgp,spkd->skgd",
        weights.astype(jnp.bfloat16),
        value_heads,
        preferred_element_type=jnp.float32,
    )
    head_cols = local_heads * group_size
    merged_top, merged_total, merged_values = combined_all(
        (
            local_top.reshape(row_count, head_cols),
            local_total.reshape(row_count, head_cols),
            local_values.reshape(row_count, head_cols * HD),
        ),
        "kv",
        combine_parts,
    )
    own_score = jnp.einsum(
        "skgd,skd->skg",
        query_heads,
        new_key.reshape(row_count, local_heads, HD),
        preferred_element_type=jnp.float32,
    ).reshape(row_count, head_cols) * HD ** (-0.5)
    final_top = jnp.maximum(merged_top, own_score)
    past_scale = jnp.exp(merged_top - final_top)
    own_weight = jnp.exp(own_score - final_top)
    totals = merged_total * past_scale + own_weight
    own_rounded = lax.optimization_barrier(own_weight.astype(jnp.bfloat16)).astype(jnp.float32)
    own_values = jnp.broadcast_to(
        new_value.astype(jnp.float32).reshape(row_count, local_heads, 1, HD),
        (row_count, local_heads, group_size, HD),
    ).reshape(row_count, head_cols * HD)
    weighted = (
        merged_values * jnp.repeat(past_scale, HD, axis=1)
        + jnp.repeat(own_rounded, HD, axis=1) * own_values
    )
    attended = (weighted / jnp.repeat(totals, HD, axis=1)).astype(jnp.bfloat16)
    partial_out = jnp.dot(attended, out_weight, preferred_element_type=jnp.float32)
    head_sum = lax.psum(partial_out.astype(jnp.bfloat16), "tp").astype(jnp.float32)
    mid_cols = (token_rows + head_sum).astype(jnp.bfloat16)
    mid_rows = lax.all_gather(mid_cols, "kv", axis=1, tiled=True)
    mid_wide = mid_rows.astype(jnp.float32)
    normed_mid = (
        mid_wide
        * mlp_gain[None, :]
        * lax.rsqrt(jnp.mean(mid_wide * mid_wide, axis=1, keepdims=True) + epsilon)
    ).astype(jnp.bfloat16)
    hidden = jnp.square(
        jax.nn.relu(jnp.dot(normed_mid, up_weight, preferred_element_type=jnp.float32))
    ).astype(jnp.bfloat16)
    mixer_term = jnp.dot(hidden, down_weight, preferred_element_type=jnp.float32)
    kv_count = lax.axis_size("kv")
    tp_count = lax.axis_size("tp")
    block_cols = mixer_term.shape[1] // (kv_count * tp_count)
    reordered = (
        mixer_term.reshape(row_count, kv_count, tp_count, block_cols)
        .transpose(0, 2, 1, 3)
        .reshape(row_count, kv_count * tp_count * block_cols)
    )
    pair_share = lax.psum_scatter(
        reordered.astype(jnp.bfloat16), "tp", scatter_dimension=1, tiled=True
    ).astype(jnp.float32)
    mixer_share = lax.psum_scatter(pair_share, "kv", scatter_dimension=1, tiled=True)
    out_cols = mixer_share.shape[1]
    start_col = (kv_place * tp_count + tp_place) * out_cols
    mid_share = lax.dynamic_slice_in_dim(mid_wide, start_col, out_cols, 1)
    return (mid_share + mixer_share).astype(jnp.bfloat16)


BF = jnp.bfloat16
F32 = jnp.float32
PAD = 8
LANES = 128
MESH = pl.DeviceIdType.MESH


def dot32(a, b):
    return jnp.dot(a, b, preferred_element_type=F32)


def layer_kernel(
    kv_n,
    tp_n,
    lengths,
    offset,
    tokens_hbm,
    gain_hbm,
    wq_hbm,
    wk_hbm,
    wv_hbm,
    fw_hbm,
    ck_hbm,
    cv_hbm,
    gate_hbm,
    wo_hbm,
    mlp_hbm,
    wu_hbm,
    wd_hbm,
    out_ref,
    tok_all,
    gain,
    wq,
    wk,
    wv,
    fw,
    ck,
    cv,
    gate,
    wo,
    mlp,
    wu,
    wd,
    rows32,
    q_own,
    q_send,
    q_recv,
    st_send,
    st_recv,
    q_heads,
    val_send,
    val_recv,
    lse_send,
    lse_recv,
    att_heads,
    part_recv,
    mid,
    hidden,
    fin_send,
    fin_recv,
    load_sem,
    up_sem,
    down_sem,
    tok_ss,
    tok_rs,
    q_ss,
    q_rs,
    st_ss,
    st_rs,
    val_ss,
    val_rs,
    lse_ss,
    lse_rs,
    part_ss,
    part_rs,
    fin_ss,
    fin_rs,
):
    dp = lax.axis_index("dp")
    z = lax.axis_index("kv")
    t = lax.axis_index("tp")
    n = kv_n * tp_n
    rows, cols = tokens_hbm.shape
    q_cols = wq.shape[1]
    kv_cols = wk.shape[1]
    here = ck.shape[1]
    chunks = q_cols // LANES
    half = LANES // 2

    def peer(r):
        dz, dt = r // tp_n, r % tp_n
        return (dp, lax.rem(z + dz, kv_n), lax.rem(t + dt, tp_n))

    barrier = pltpu.get_barrier_semaphore()
    for r in range(1, n):
        pl.semaphore_signal(barrier, inc=1, device_id=peer(r), device_id_type=MESH)

    loads = {}

    def load(name, source, target):
        copy = pltpu.make_async_copy(source, target, load_sem.at[len(loads)])
        copy.start()
        loads[name] = copy

    load("tokens", tokens_hbm, tok_all.at[z])
    load("gain", gain_hbm, gain)
    load("wq", wq_hbm, wq)
    load("wk", wk_hbm, wk)
    load("wv", wv_hbm, wv)
    load("fw", fw_hbm, fw)
    load("ck", ck_hbm, ck)
    load("gate", gate_hbm, gate)
    load("cv", cv_hbm, cv)
    load("wo0", wo_hbm.at[0], wo.at[:, 0])
    load("wo1", wo_hbm.at[1], wo.at[:, 1])
    load("mlp", mlp_hbm, mlp)

    up_tile = hidden.shape[1] // up_sem.shape[0]

    def up_copy(j):
        span = pl.ds(pl.multiple_of(j * up_tile, LANES), up_tile)
        return pltpu.make_async_copy(wu_hbm.at[:, span], wu.at[:, span], up_sem.at[j])

    def down_span(r):
        _, pz, pt = peer(r)
        width = fin_send.shape[2]
        return pl.ds(pl.multiple_of((pz * tp_n + pt) * width, LANES), width)

    def down_copy(r):
        span = down_span(r)
        return pltpu.make_async_copy(wd_hbm.at[:, span], wd.at[:, span], down_sem.at[r])

    for j in range(up_sem.shape[0]):
        up_copy(j).start()
    for r in reversed(range(n)):
        down_copy(r).start()

    def send(source, target, ss, rs, r):
        copy = pltpu.make_async_remote_copy(
            src_ref=source,
            dst_ref=target,
            send_sem=ss,
            recv_sem=rs,
            device_id=peer(r),
            device_id_type=MESH,
        )
        copy.start()
        return copy

    rows32[...] = jnp.zeros_like(rows32)
    loads["tokens"].wait()
    loads["gain"].wait()
    rows32[0:rows, :] = tok_all[z].astype(F32)
    own_rows = rows32[...]
    scaled = (own_rows * gain[...]).astype(BF)
    scaled32 = scaled.astype(F32)
    loads["fw"].wait()
    fw_here = fw[:, pl.ds(pl.multiple_of(z * cols, LANES), cols)].astype(F32)
    lane = lax.broadcasted_iota(jnp.int32, (PAD, LANES), 1)
    stats = jnp.where(
        lane == KEY_VALUE_HEADS, jnp.sum(own_rows * own_rows, axis=1, keepdims=True), 0.0
    )
    for h in range(KEY_VALUE_HEADS):
        part = jnp.sum(scaled32 * fw_here[h : h + 1, :], axis=1, keepdims=True)
        stats = jnp.where(lane == h, part, stats)
    st_send[...] = stats

    loads["wq"].wait()
    q_tile = 512 if q_cols % 512 == 0 else LANES

    @pl.loop(0, q_cols // q_tile)
    def _(j):
        span = pl.ds(pl.multiple_of(j * q_tile, LANES), q_tile)
        part = dot32(scaled, wq[:, span])
        q_own[:, span] = part
        q_send[:, span] = part.astype(BF)

    loads["wk"].wait()
    loads["wv"].wait()
    for place, weight in ((q_cols, wk), (q_cols + kv_cols, wv)):
        part = dot32(scaled, weight[...])
        q_own[:, place : place + kv_cols] = part
        q_send[:, place : place + kv_cols] = part.astype(BF)

    pl.semaphore_wait(barrier, n - 1)
    sent = []
    q_copies, val_copies = [], []
    for dz in reversed(range(1, kv_n)):
        r = dz * tp_n
        k = dz - 1
        q_copies.append(send(q_send, q_recv.at[k], q_ss.at[k], q_rs.at[k], r))
        q_copies.append(send(st_send, st_recv.at[k], st_ss.at[k], st_rs.at[k], r))
    tok_copies = []
    for dz in range(1, kv_n):
        k = dz - 1
        tok_copies.append(
            send(tok_all.at[z], tok_all.at[z], tok_ss.at[k], tok_rs.at[k], dz * tp_n)
        )
    for copy in q_copies:
        copy.wait_recv()
    q_sum = q_own[...]
    st_sum = st_send[...]
    for k in range(kv_n - 1):
        q_sum = q_sum + q_recv[k].astype(F32)
        st_sum = st_sum + st_recv[k]
    square = st_sum[:, KEY_VALUE_HEADS : KEY_VALUE_HEADS + 1]
    row_scale = lax.rsqrt(square / (cols * kv_n) + epsilon)
    q_sum = (q_sum * row_scale).astype(BF).astype(F32)
    for c in range(chunks):
        q_heads[c] = q_sum[:, c * LANES : (c + 1) * LANES]
    new_key = q_sum[:, q_cols : q_cols + kv_cols]
    new_value = q_sum[:, q_cols + kv_cols :]
    local = KEY_VALUE_HEADS // tp_n
    forgets = []
    for g in range(local):
        raw = st_sum[:, g : g + 1]
        for other in range(1, tp_n):
            at = other * local + g
            raw = jnp.where(t == other, st_sum[:, at : at + 1], raw)
        x = raw * row_scale + offset[g]
        forgets.append(jnp.minimum(x, 0.0) - jnp.log(1.0 + jnp.exp(-jnp.abs(x))))

    scale = HD ** (-0.5)
    low8 = lax.broadcasted_iota(jnp.int32, (chunks // 2, LANES), 1) < half
    lane16 = lax.broadcasted_iota(jnp.int32, (chunks, LANES), 1)
    low16 = lane16 < half
    position = z * here + lax.broadcasted_iota(jnp.int32, (2 * chunks, here), 1)
    loads["ck"].wait()
    loads["gate"].wait()
    loads["cv"].wait()
    lse_all = jnp.zeros((chunks, LANES), F32)
    own_scores, own_lse, own_vals = [], [], []
    hc = chunks // 2
    for b in range(rows):
        x = q_heads[:, b, :]
        turned = pltpu.roll(x, half, 1)
        spread = jnp.concatenate(
            [
                jnp.where(low8, x[:hc], 0.0),
                jnp.where(low8, turned[:hc], 0.0),
                jnp.where(low8, 0.0, turned[hc:]),
                jnp.where(low8, 0.0, x[hc:]),
            ],
            axis=0,
        )
        own = jnp.sum(spread * new_key[b : b + 1, :], axis=1, keepdims=True) * scale
        own_scores.append(jnp.where(low16, own[:chunks], own[chunks:]))
        scores = scale * lax.dot_general(
            spread.astype(BF), ck[b], (((1,), (1,)), ((), ())), preferred_element_type=F32
        )
        bias = jnp.concatenate(
            [
                jnp.broadcast_to(gate[b, g : g + 1, :] + forgets[g][b : b + 1, :], (chunks, here))
                for g in range(local)
            ],
            axis=0,
        )
        live = position < lengths[b]
        scores = jnp.where(live, scores + bias, floor_score)
        top = jnp.max(scores, axis=1, keepdims=True)
        weights = jnp.where(live, jnp.exp(scores - top), 0.0)
        total = jnp.maximum(jnp.sum(weights, axis=1, keepdims=True), 1e-30)
        vals = dot32(weights.astype(BF), cv[b]) / total
        lse = top + jnp.log(total)
        lse = jnp.where(low16, lse[:chunks], lse[chunks:])
        vals = jnp.where(low16, vals[:chunks], vals[chunks:])
        own_lse.append(lse)
        own_vals.append(vals)
        lse_all = jnp.where((lane16 & (half - 1)) == b, lse, lse_all)
        val_send[b * chunks : (b + 1) * chunks, :] = vals.astype(BF)
    lse_send[...] = lse_all
    for dz in reversed(range(1, kv_n)):
        r = dz * tp_n
        k = dz - 1
        val_copies.append(send(val_send, val_recv.at[k], val_ss.at[k], val_rs.at[k], r))
        val_copies.append(send(lse_send, lse_recv.at[k], lse_ss.at[k], lse_rs.at[k], r))
    att_heads[...] = jnp.zeros_like(att_heads)
    for copy in val_copies:
        copy.wait_recv()
    for b in range(rows):
        levels = [own_scores[b], own_lse[b]]
        terms = [jnp.broadcast_to(new_value[b : b + 1, :], (chunks, LANES)), own_vals[b]]
        for k in range(kv_n - 1):
            got = lse_recv[k]
            levels.append(
                jnp.where(low16, got[:, b : b + 1], got[:, half + b : half + b + 1])
            )
            terms.append(val_recv[k, b * chunks : (b + 1) * chunks, :].astype(F32))
        peak = functools.reduce(jnp.maximum, levels)
        bottom = jnp.zeros((chunks, LANES), F32)
        upper = jnp.zeros((chunks, LANES), F32)
        for level, term in zip(levels, terms):
            share = jnp.exp(level - peak)
            bottom = bottom + share
            upper = upper + share * term
        att_heads[:, b, :] = upper / bottom

    order = [c // 2 + (c % 2) * hc for c in range(chunks)]
    attended = jnp.concatenate([att_heads[c] for c in order], axis=1).astype(BF)
    loads["wo0"].wait()
    loads["wo1"].wait()
    o_tile = 256 if cols % 256 == 0 else LANES
    for j in range(cols // o_tile):
        weight = wo[:, :, :, j * o_tile : (j + 1) * o_tile].reshape(q_cols, o_tile)
        part_recv[z, t, :, j * o_tile : (j + 1) * o_tile] = dot32(attended, weight).astype(BF)
    part_copies = []
    for r in reversed(range(1, n)):
        part_copies.append(
            send(part_recv.at[z, t], part_recv.at[z, t], part_ss.at[r], part_rs.at[r], r)
        )
    for copy in tok_copies:
        copy.wait_recv()
    for copy in part_copies:
        copy.wait_recv()
    mid[...] = jnp.zeros_like(mid)
    for s in range(kv_n):
        mid[0:rows, s * cols : (s + 1) * cols] = tok_all[s].astype(F32)
    for s in range(kv_n):
        span = slice(s * cols, (s + 1) * cols)
        total = mid[:, span]
        for g in range(tp_n):
            total = total + part_recv[s, g].astype(F32)
        mid[:, span] = total.astype(BF).astype(F32)

    wide = mid[...]
    loads["mlp"].wait()
    inverse = lax.rsqrt(jnp.mean(wide * wide, axis=1, keepdims=True) + epsilon)
    normed = (wide * mlp[...] * inverse).astype(BF)

    @pl.loop(0, up_sem.shape[0])
    def _(j):
        up_copy(j).wait()
        span = pl.ds(pl.multiple_of(j * up_tile, LANES), up_tile)
        hot = jnp.maximum(dot32(normed, wu[:, span]), 0.0)
        hidden[:, span] = (hot * hot).astype(BF)

    def fin_copy(r):
        return pltpu.make_async_remote_copy(
            src_ref=fin_send.at[r],
            dst_ref=fin_recv.at[r],
            send_sem=fin_ss.at[r],
            recv_sem=fin_rs.at[r],
            device_id=peer(r),
            device_id_type=MESH,
        )

    active = hidden[...]

    @pl.loop(0, n - 1)
    def _(i):
        r = n - 1 - i
        down_copy(r).wait()
        fin_send[r] = dot32(active, wd[:, down_span(r)]).astype(BF)
        fin_copy(r).start()

    down_copy(0).wait()
    result = dot32(active, wd[:, down_span(0)]) + mid[:, down_span(0)]
    for r in reversed(range(1, n)):
        fin_copy(r).wait_recv()
        result = result + fin_recv[r].astype(F32)
    out_ref[...] = result[0:rows, :].astype(BF)
    for copy in q_copies + tok_copies + val_copies + part_copies:
        copy.wait_send()
    for r in range(1, n):
        fin_copy(r).wait_send()


def kernel_shards(
    kv_n,
    tp_n,
    tokens,
    lengths,
    attn_gain,
    query_weight,
    key_weight,
    value_weight,
    forget_weight,
    forget_offset,
    cache_keys,
    cache_values,
    gate_sum,
    out_weight,
    mlp_gain,
    up_weight,
    down_weight,
):
    rows, cols = tokens.shape
    n = kv_n * tp_n
    q_cols = query_weight.shape[1]
    kv_cols = key_weight.shape[1]
    chunks = q_cols // LANES
    local = kv_cols // HD
    units = up_weight.shape[1]
    width = down_weight.shape[1]
    out_cols = width // n
    out_blocks = out_weight.reshape(local, chunks, HD, cols)
    up_tiles = 4
    peers = kv_n - 1
    vm = pltpu.VMEM
    dma = pltpu.SemaphoreType.DMA
    any_spec = pl.BlockSpec(memory_space=pl.ANY)
    smem_spec = pl.BlockSpec(memory_space=pltpu.SMEM)
    moved = (
        tokens,
        attn_gain.reshape(1, cols),
        query_weight,
        key_weight,
        value_weight,
        forget_weight.T,
        cache_keys,
        cache_values,
        gate_sum,
        out_blocks,
        mlp_gain.reshape(1, width),
        up_weight,
        down_weight,
    )
    scratch = [
        vm((kv_n, rows, cols), BF),
        vm((1, cols), F32),
        vm(query_weight.shape, BF),
        vm(key_weight.shape, BF),
        vm(value_weight.shape, BF),
        vm(forget_weight.shape[::-1], BF),
        vm(cache_keys.shape, BF),
        vm(cache_values.shape, BF),
        vm(gate_sum.shape, F32),
        vm((chunks, local, HD, cols), BF),
        vm((1, width), F32),
        vm(up_weight.shape, BF),
        vm(down_weight.shape, BF),
        vm((PAD, cols), F32),
        vm((PAD, q_cols + 2 * kv_cols), F32),
        vm((PAD, q_cols + 2 * kv_cols), BF),
        vm((peers, PAD, q_cols + 2 * kv_cols), BF),
        vm((PAD, LANES), F32),
        vm((peers, PAD, LANES), F32),
        vm((chunks, PAD, LANES), F32),
        vm((rows * chunks, LANES), BF),
        vm((peers, rows * chunks, LANES), BF),
        vm((chunks, LANES), F32),
        vm((peers, chunks, LANES), F32),
        vm((chunks, PAD, LANES), F32),
        vm((kv_n, tp_n, PAD, cols), BF),
        vm((PAD, width), F32),
        vm((PAD, units), BF),
        vm((n, PAD, out_cols), BF),
        vm((n, PAD, out_cols), BF),
        dma((12,)),
        dma((up_tiles,)),
        dma((n,)),
    ]
    for count in (peers, peers, peers, peers, peers, n, n):
        scratch += [dma((count,)), dma((count,))]
    return pl.pallas_call(
        functools.partial(layer_kernel, kv_n, tp_n),
        out_shape=jax.ShapeDtypeStruct((rows, out_cols), BF),
        in_specs=[smem_spec] * 2 + [any_spec] * len(moved),
        out_specs=pl.BlockSpec(memory_space=pltpu.VMEM),
        scratch_shapes=scratch,
        compiler_params=pltpu.CompilerParams(
            collective_id=0, has_side_effects=True, vmem_limit_bytes=60 * 1024 * 1024
        ),
        name="layer",
    )(lengths, forget_offset, *moved)


def fits(kv_n, tp_n, tokens, query_weight, key_weight, forget_weight, up_weight, down_weight):
    rows, cols = tokens.shape
    held = 4 * query_weight.size + up_weight.size * 2 + down_weight.size * 2
    return (
        rows <= PAD
        and kv_n > 1
        and cols % LANES == 0
        and key_weight.shape[1] == LANES
        and HD * 2 == LANES
        and up_weight.shape[1] % (4 * LANES) == 0
        and down_weight.shape[1] % (kv_n * tp_n * LANES) == 0
        and held < 48 * 1024 * 1024
    )


def shards(*args):
    kv_n = lax.axis_size("kv")
    tp_n = lax.axis_size("tp")
    if fits(kv_n, tp_n, args[0], args[3], args[4], args[6], args[13], args[14]):
        return kernel_shards(kv_n, tp_n, *args)
    return general_shards(*args)


def solution(mesh):
    placed = (
        P("dp", "kv"),
        P("dp"),
        P("kv"),
        P("kv", "tp"),
        P("kv", "tp"),
        P("kv", "tp"),
        P(),
        P("tp"),
        P("dp", "kv", "tp"),
        P("dp", "kv", "tp"),
        P("dp", "tp", "kv"),
        P("tp", "kv"),
        P(),
        P(None, ("kv", "tp")),
        P(("kv", "tp"), None),
    )
    return jax.shard_map(
        shards, mesh=mesh, in_specs=placed, out_specs=P("dp", ("kv", "tp")), check_vma=False
    )
```

```python
import functools

import jax
import jax.numpy as jnp
from jax import lax
from jax.experimental import pallas as pl
from jax.experimental.pallas import tpu as pltpu
from jax.sharding import PartitionSpec as P

D = 4096
HEADS = 64
HD = 64
KEY_VALUE_HEADS = 4


epsilon = 1e-06
floor_score = -1e30


def combined_all(x, axis, combine):
    everything = jax.tree.map(
        lambda part, kind: lax.all_gather(part.astype(kind), axis),
        x,
        (jnp.bfloat16, jnp.bfloat16, jnp.bfloat16),
    )

    def take(k):
        return jax.tree.map(lambda part, own: part[k].astype(own.dtype), everything, x)

    return lax.fori_loop(
        1, lax.axis_size(axis), lambda k, so_far: combine(so_far, take(k)), take(0)
    )


def combine_parts(earlier, later):
    first_top, first_total, first_values = earlier
    second_top, second_total, second_values = later
    merged_top = jnp.maximum(first_top, second_top)
    first_scale = jnp.exp(first_top - merged_top)
    second_scale = jnp.exp(second_top - merged_top)
    first_wide = jnp.repeat(first_scale, HD, axis=1)
    second_wide = jnp.repeat(second_scale, HD, axis=1)
    return (
        merged_top,
        first_total * first_scale + second_total * second_scale,
        first_values * first_wide + second_values * second_wide,
    )


def general_shards(
    tokens,
    lengths,
    attn_gain,
    query_weight,
    key_weight,
    value_weight,
    forget_weight,
    forget_offset,
    cache_keys,
    cache_values,
    gate_sum,
    out_weight,
    mlp_gain,
    up_weight,
    down_weight,
):
    row_count = tokens.shape[0]
    feature_cols = tokens.shape[1]
    kv_place = lax.axis_index("kv")
    tp_place = lax.axis_index("tp")
    local_heads = key_weight.shape[1] // HD
    group_size = HEADS // KEY_VALUE_HEADS
    token_rows = tokens.astype(jnp.float32)
    scaled_rows = (token_rows * attn_gain[None, :]).astype(jnp.bfloat16)
    square_part = jnp.sum(token_rows * token_rows, axis=1)
    query_part = jnp.dot(scaled_rows, query_weight, preferred_element_type=jnp.float32)
    key_part = jnp.dot(scaled_rows, key_weight, preferred_element_type=jnp.float32)
    value_part = jnp.dot(scaled_rows, value_weight, preferred_element_type=jnp.float32)
    gate_rows = lax.dynamic_slice(
        forget_weight,
        (kv_place * feature_cols, tp_place * local_heads),
        (feature_cols, local_heads),
    )
    forget_part = jnp.dot(scaled_rows, gate_rows, preferred_element_type=jnp.float32)
    query_sum, key_sum, value_sum, forget_sum, square_sum = lax.psum(
        (query_part, key_part, value_part, forget_part, square_part), "kv"
    )
    row_scale = lax.rsqrt(square_sum / D + epsilon)[:, None]
    queries = (query_sum * row_scale).astype(jnp.bfloat16)
    new_key = (key_sum * row_scale).astype(jnp.bfloat16)
    new_value = (value_sum * row_scale).astype(jnp.bfloat16)
    log_forget = jax.nn.log_sigmoid(forget_sum * row_scale + forget_offset[None, :])
    positions_here = cache_keys.shape[1]
    key_heads = cache_keys.reshape(row_count, positions_here, local_heads, HD)
    value_heads = cache_values.reshape(row_count, positions_here, local_heads, HD)
    query_heads = queries.reshape(row_count, local_heads, group_size, HD)
    scores = jnp.einsum(
        "skgd,spkd->skgp", query_heads, key_heads, preferred_element_type=jnp.float32
    ) * HD ** (-0.5)
    scores = scores + gate_sum[:, :, None, :] + log_forget[:, :, None, None]
    cache_pos = kv_place * positions_here + jnp.arange(positions_here)
    active_mask = (cache_pos[None, :] < lengths[:, None])[:, None, None, :]
    local_top = jnp.max(jnp.where(active_mask, scores, floor_score), axis=3)
    weights = jnp.where(active_mask, jnp.exp(scores - local_top[..., None]), 0.0)
    local_total = jnp.sum(weights, axis=3)
    local_values = jnp.einsum(
        "skgp,spkd->skgd",
        weights.astype(jnp.bfloat16),
        value_heads,
        preferred_element_type=jnp.float32,
    )
    head_cols = local_heads * group_size
    merged_top, merged_total, merged_values = combined_all(
        (
            local_top.reshape(row_count, head_cols),
            local_total.reshape(row_count, head_cols),
            local_values.reshape(row_count, head_cols * HD),
        ),
        "kv",
        combine_parts,
    )
    own_score = jnp.einsum(
        "skgd,skd->skg",
        query_heads,
        new_key.reshape(row_count, local_heads, HD),
        preferred_element_type=jnp.float32,
    ).reshape(row_count, head_cols) * HD ** (-0.5)
    final_top = jnp.maximum(merged_top, own_score)
    past_scale = jnp.exp(merged_top - final_top)
    own_weight = jnp.exp(own_score - final_top)
    totals = merged_total * past_scale + own_weight
    own_rounded = lax.optimization_barrier(own_weight.astype(jnp.bfloat16)).astype(jnp.float32)
    own_values = jnp.broadcast_to(
        new_value.astype(jnp.float32).reshape(row_count, local_heads, 1, HD),
        (row_count, local_heads, group_size, HD),
    ).reshape(row_count, head_cols * HD)
    weighted = (
        merged_values * jnp.repeat(past_scale, HD, axis=1)
        + jnp.repeat(own_rounded, HD, axis=1) * own_values
    )
    attended = (weighted / jnp.repeat(totals, HD, axis=1)).astype(jnp.bfloat16)
    partial_out = jnp.dot(attended, out_weight, preferred_element_type=jnp.float32)
    head_sum = lax.psum(partial_out.astype(jnp.bfloat16), "tp").astype(jnp.float32)
    mid_cols = (token_rows + head_sum).astype(jnp.bfloat16)
    mid_rows = lax.all_gather(mid_cols, "kv", axis=1, tiled=True)
    mid_wide = mid_rows.astype(jnp.float32)
    normed_mid = (
        mid_wide
        * mlp_gain[None, :]
        * lax.rsqrt(jnp.mean(mid_wide * mid_wide, axis=1, keepdims=True) + epsilon)
    ).astype(jnp.bfloat16)
    hidden = jnp.square(
        jax.nn.relu(jnp.dot(normed_mid, up_weight, preferred_element_type=jnp.float32))
    ).astype(jnp.bfloat16)
    mixer_term = jnp.dot(hidden, down_weight, preferred_element_type=jnp.float32)
    kv_count = lax.axis_size("kv")
    tp_count = lax.axis_size("tp")
    block_cols = mixer_term.shape[1] // (kv_count * tp_count)
    reordered = (
        mixer_term.reshape(row_count, kv_count, tp_count, block_cols)
        .transpose(0, 2, 1, 3)
        .reshape(row_count, kv_count * tp_count * block_cols)
    )
    pair_share = lax.psum_scatter(
        reordered.astype(jnp.bfloat16), "tp", scatter_dimension=1, tiled=True
    ).astype(jnp.float32)
    mixer_share = lax.psum_scatter(pair_share, "kv", scatter_dimension=1, tiled=True)
    out_cols = mixer_share.shape[1]
    start_col = (kv_place * tp_count + tp_place) * out_cols
    mid_share = lax.dynamic_slice_in_dim(mid_wide, start_col, out_cols, 1)
    return (mid_share + mixer_share).astype(jnp.bfloat16)


BF = jnp.bfloat16
F32 = jnp.float32
PAD = 8
LANES = 128
MESH = pl.DeviceIdType.MESH


def dot32(a, b):
    return jnp.dot(a, b, preferred_element_type=F32)


def layer_kernel(
    kv_n,
    tp_n,
    lengths,
    offset,
    tokens_hbm,
    gain_hbm,
    wq_hbm,
    wk_hbm,
    wv_hbm,
    fw_hbm,
    ck_hbm,
    cv_hbm,
    gate_hbm,
    wo_hbm,
    mlp_hbm,
    wu_hbm,
    wd_hbm,
    out_ref,
    tok_in,
    gain,
    wq,
    wk,
    wv,
    fw,
    ck,
    cv,
    gate,
    wo,
    mlp,
    wu,
    wd,
    rows32,
    q_own,
    q_send,
    q_recv,
    st_send,
    st_recv,
    q_heads,
    val_send,
    val_recv,
    lse_send,
    lse_recv,
    att_heads,
    part_recv,
    mid,
    hidden,
    fin_send,
    fin_recv,
    load_sem,
    up_sem,
    down_sem,
    q_ss,
    q_rs,
    st_ss,
    st_rs,
    val_ss,
    val_rs,
    lse_ss,
    lse_rs,
    part_ss,
    part_rs,
    fin_ss,
    fin_rs,
):
    dp = lax.axis_index("dp")
    z = lax.axis_index("kv")
    t = lax.axis_index("tp")
    n = kv_n * tp_n
    rows, cols = tokens_hbm.shape
    q_cols = wq.shape[1]
    kv_cols = wk.shape[1]
    here = ck.shape[1]
    chunks = q_cols // LANES
    half = LANES // 2

    def peer(r):
        dz, dt = r // tp_n, r % tp_n
        return (dp, lax.rem(z + dz, kv_n), lax.rem(t + dt, tp_n))

    barrier = pltpu.get_barrier_semaphore()
    for r in range(1, n):
        pl.semaphore_signal(barrier, inc=1, device_id=peer(r), device_id_type=MESH)

    loads = {}

    def load(name, source, target):
        copy = pltpu.make_async_copy(source, target, load_sem.at[len(loads)])
        copy.start()
        loads[name] = copy

    load("tokens", tokens_hbm, tok_in)
    load("gain", gain_hbm, gain)
    load("fw", fw_hbm, fw)
    q_pieces = q_ss.shape[0]
    piece = q_cols // q_pieces
    for j in range(q_pieces):
        load(f"wq{j}", wq_hbm.at[:, pl.ds(j * piece, piece)], wq.at[:, pl.ds(j * piece, piece)])
    load("wk", wk_hbm, wk)
    load("wv", wv_hbm, wv)
    load("ck", ck_hbm, ck)
    load("gate", gate_hbm, gate)
    load("cv", cv_hbm, cv)
    load("wo0", wo_hbm.at[0], wo.at[:, 0])
    load("wo1", wo_hbm.at[1], wo.at[:, 1])
    load("mlp", mlp_hbm, mlp)

    up_tile = hidden.shape[1] // up_sem.shape[0]

    def up_copy(j):
        span = pl.ds(pl.multiple_of(j * up_tile, LANES), up_tile)
        return pltpu.make_async_copy(wu_hbm.at[:, span], wu.at[:, span], up_sem.at[j])

    def down_span(r):
        _, pz, pt = peer(r)
        width = fin_send.shape[2]
        return pl.ds(pl.multiple_of((pz * tp_n + pt) * width, LANES), width)

    def down_copy(r):
        span = down_span(r)
        return pltpu.make_async_copy(wd_hbm.at[:, span], wd.at[:, span], down_sem.at[r])

    for j in range(up_sem.shape[0]):
        up_copy(j).start()
    for r in reversed(range(n)):
        down_copy(r).start()

    def send(source, target, ss, rs, r):
        copy = pltpu.make_async_remote_copy(
            src_ref=source,
            dst_ref=target,
            send_sem=ss,
            recv_sem=rs,
            device_id=peer(r),
            device_id_type=MESH,
        )
        copy.start()
        return copy

    rows32[...] = jnp.zeros_like(rows32)
    loads["tokens"].wait()
    loads["gain"].wait()
    rows32[0:rows, :] = tok_in[...].astype(F32)
    own_rows = rows32[...]
    scaled = (own_rows * gain[...]).astype(BF)
    scaled32 = scaled.astype(F32)
    loads["fw"].wait()
    fw_here = fw[:, pl.ds(pl.multiple_of(z * cols, LANES), cols)].astype(F32)
    lane = lax.broadcasted_iota(jnp.int32, (PAD, LANES), 1)
    stats = jnp.where(
        lane == KEY_VALUE_HEADS, jnp.sum(own_rows * own_rows, axis=1, keepdims=True), 0.0
    )
    for h in range(KEY_VALUE_HEADS):
        part = jnp.sum(scaled32 * fw_here[h : h + 1, :], axis=1, keepdims=True)
        stats = jnp.where(lane == h, part, stats)
    st_send[...] = stats

    q_copies, val_copies = [], []
    for j in range(q_pieces):
        loads[f"wq{j}"].wait()
        span = pl.ds(j * piece, piece)
        part = dot32(scaled, wq[:, span])
        q_own[:, span] = part
        q_send[:, span] = part.astype(BF)
        if j == q_pieces - 1:
            loads["wk"].wait()
            loads["wv"].wait()
            for place, weight in ((q_cols, wk), (q_cols + kv_cols, wv)):
                part = dot32(scaled, weight[...])
                q_own[:, place : place + kv_cols] = part
                q_send[:, place : place + kv_cols] = part.astype(BF)
            span = pl.ds(j * piece, piece + 2 * kv_cols)
        if j == 0:
            pl.semaphore_wait(barrier, n - 1)
            for dz in reversed(range(1, kv_n)):
                k = dz - 1
                q_copies.append(
                    send(st_send, st_recv.at[k], st_ss.at[k], st_rs.at[k], dz * tp_n)
                )
        for dz in reversed(range(1, kv_n)):
            k = dz - 1
            q_copies.append(
                send(
                    q_send.at[:, span],
                    q_recv.at[k, :, span],
                    q_ss.at[j, k],
                    q_rs.at[j, k],
                    dz * tp_n,
                )
            )
    for copy in q_copies:
        copy.wait_recv()
    q_sum = q_own[...]
    st_sum = st_send[...]
    for k in range(kv_n - 1):
        q_sum = q_sum + q_recv[k].astype(F32)
        st_sum = st_sum + st_recv[k]
    square = st_sum[:, KEY_VALUE_HEADS : KEY_VALUE_HEADS + 1]
    row_scale = lax.rsqrt(square / (cols * kv_n) + epsilon)
    q_sum = (q_sum * row_scale).astype(BF).astype(F32)
    for c in range(chunks):
        q_heads[c] = q_sum[:, c * LANES : (c + 1) * LANES]
    new_key = q_sum[:, q_cols : q_cols + kv_cols]
    new_value = q_sum[:, q_cols + kv_cols :]
    local = KEY_VALUE_HEADS // tp_n
    forgets = []
    for g in range(local):
        raw = st_sum[:, g : g + 1]
        for other in range(1, tp_n):
            at = other * local + g
            raw = jnp.where(t == other, st_sum[:, at : at + 1], raw)
        x = raw * row_scale + offset[g]
        forgets.append(jnp.minimum(x, 0.0) - jnp.log(1.0 + jnp.exp(-jnp.abs(x))))

    scale = HD ** (-0.5)
    low8 = lax.broadcasted_iota(jnp.int32, (chunks // 2, LANES), 1) < half
    lane16 = lax.broadcasted_iota(jnp.int32, (chunks, LANES), 1)
    low16 = lane16 < half
    position = z * here + lax.broadcasted_iota(jnp.int32, (2 * chunks, here), 1)
    loads["ck"].wait()
    loads["gate"].wait()
    loads["cv"].wait()
    lse_all = jnp.zeros((chunks, LANES), F32)
    own_scores, own_lse, own_vals = [], [], []
    hc = chunks // 2
    for b in range(rows):
        x = q_heads[:, b, :]
        turned = pltpu.roll(x, half, 1)
        spread = jnp.concatenate(
            [
                jnp.where(low8, x[:hc], 0.0),
                jnp.where(low8, turned[:hc], 0.0),
                jnp.where(low8, 0.0, turned[hc:]),
                jnp.where(low8, 0.0, x[hc:]),
            ],
            axis=0,
        )
        own = jnp.sum(spread * new_key[b : b + 1, :], axis=1, keepdims=True) * scale
        own_scores.append(jnp.where(low16, own[:chunks], own[chunks:]))
        scores = scale * lax.dot_general(
            spread.astype(BF), ck[b], (((1,), (1,)), ((), ())), preferred_element_type=F32
        )
        bias = jnp.concatenate(
            [
                jnp.broadcast_to(gate[b, g : g + 1, :] + forgets[g][b : b + 1, :], (chunks, here))
                for g in range(local)
            ],
            axis=0,
        )
        live = position < lengths[b]
        scores = jnp.where(live, scores + bias, floor_score)
        top = jnp.max(scores, axis=1, keepdims=True)
        weights = jnp.where(live, jnp.exp(scores - top), 0.0)
        total = jnp.maximum(jnp.sum(weights, axis=1, keepdims=True), 1e-30)
        vals = dot32(weights.astype(BF), cv[b]) / total
        lse = top + jnp.log(total)
        lse = jnp.where(low16, lse[:chunks], lse[chunks:])
        vals = jnp.where(low16, vals[:chunks], vals[chunks:])
        own_lse.append(lse)
        own_vals.append(vals)
        lse_all = jnp.where((lane16 & (half - 1)) == b, lse, lse_all)
        val_send[b * chunks : (b + 1) * chunks, :] = vals.astype(BF)
    lse_send[...] = lse_all
    for dz in reversed(range(1, kv_n)):
        r = dz * tp_n
        k = dz - 1
        val_copies.append(send(val_send, val_recv.at[k], val_ss.at[k], val_rs.at[k], r))
        val_copies.append(send(lse_send, lse_recv.at[k], lse_ss.at[k], lse_rs.at[k], r))
    att_heads[...] = jnp.zeros_like(att_heads)
    for copy in val_copies:
        copy.wait_recv()
    for b in range(rows):
        levels = [own_scores[b], own_lse[b]]
        terms = [jnp.broadcast_to(new_value[b : b + 1, :], (chunks, LANES)), own_vals[b]]
        for k in range(kv_n - 1):
            got = lse_recv[k]
            levels.append(
                jnp.where(low16, got[:, b : b + 1], got[:, half + b : half + b + 1])
            )
            terms.append(val_recv[k, b * chunks : (b + 1) * chunks, :].astype(F32))
        peak = functools.reduce(jnp.maximum, levels)
        bottom = jnp.zeros((chunks, LANES), F32)
        upper = jnp.zeros((chunks, LANES), F32)
        for level, term in zip(levels, terms):
            share = jnp.exp(level - peak)
            bottom = bottom + share
            upper = upper + share * term
        att_heads[:, b, :] = upper / bottom

    order = [c // 2 + (c % 2) * hc for c in range(chunks)]
    attended = jnp.concatenate([att_heads[c] for c in order], axis=1).astype(BF)
    loads["wo0"].wait()
    loads["wo1"].wait()
    residual = jnp.where(t == 0, rows32[...], 0.0)
    o_tile = 256 if cols % 256 == 0 else LANES
    for j in range(cols // o_tile):
        weight = wo[:, :, :, j * o_tile : (j + 1) * o_tile].reshape(q_cols, o_tile)
        share = dot32(attended, weight) + residual[:, j * o_tile : (j + 1) * o_tile]
        part_recv[z, t, :, j * o_tile : (j + 1) * o_tile] = share.astype(BF)
    part_copies = []
    for r in reversed(range(1, n)):
        part_copies.append(
            send(part_recv.at[z, t], part_recv.at[z, t], part_ss.at[r], part_rs.at[r], r)
        )
    for copy in part_copies:
        copy.wait_recv()
    for s in range(kv_n):
        total = part_recv[s, 0].astype(F32)
        for g in range(1, tp_n):
            total = total + part_recv[s, g].astype(F32)
        mid[:, s * cols : (s + 1) * cols] = total.astype(BF).astype(F32)

    wide = mid[...]
    loads["mlp"].wait()
    inverse = lax.rsqrt(jnp.mean(wide * wide, axis=1, keepdims=True) + epsilon)
    normed = (wide * mlp[...] * inverse).astype(BF)

    @pl.loop(0, up_sem.shape[0])
    def _(j):
        up_copy(j).wait()
        span = pl.ds(pl.multiple_of(j * up_tile, LANES), up_tile)
        hot = jnp.maximum(dot32(normed, wu[:, span]), 0.0)
        hidden[:, span] = (hot * hot).astype(BF)

    def fin_copy(r):
        return pltpu.make_async_remote_copy(
            src_ref=fin_send.at[r],
            dst_ref=fin_recv.at[r],
            send_sem=fin_ss.at[r],
            recv_sem=fin_rs.at[r],
            device_id=peer(r),
            device_id_type=MESH,
        )

    active = hidden[...]

    @pl.loop(0, n - 1)
    def _(i):
        r = n - 1 - i
        down_copy(r).wait()
        fin_send[r] = dot32(active, wd[:, down_span(r)]).astype(BF)
        fin_copy(r).start()

    down_copy(0).wait()
    result = dot32(active, wd[:, down_span(0)]) + mid[:, down_span(0)]
    for r in reversed(range(1, n)):
        fin_copy(r).wait_recv()
        result = result + fin_recv[r].astype(F32)
    out_ref[...] = result[0:rows, :].astype(BF)
    for copy in q_copies + val_copies + part_copies:
        copy.wait_send()
    for r in range(1, n):
        fin_copy(r).wait_send()


def kernel_shards(
    kv_n,
    tp_n,
    tokens,
    lengths,
    attn_gain,
    query_weight,
    key_weight,
    value_weight,
    forget_weight,
    forget_offset,
    cache_keys,
    cache_values,
    gate_sum,
    out_weight,
    mlp_gain,
    up_weight,
    down_weight,
):
    rows, cols = tokens.shape
    n = kv_n * tp_n
    q_cols = query_weight.shape[1]
    kv_cols = key_weight.shape[1]
    chunks = q_cols // LANES
    local = kv_cols // HD
    units = up_weight.shape[1]
    width = down_weight.shape[1]
    out_cols = width // n
    out_blocks = out_weight.reshape(local, chunks, HD, cols)
    up_tiles = 4
    pieces = 2 if q_cols % (2 * LANES) == 0 else 1
    peers = kv_n - 1
    vm = pltpu.VMEM
    dma = pltpu.SemaphoreType.DMA
    any_spec = pl.BlockSpec(memory_space=pl.ANY)
    smem_spec = pl.BlockSpec(memory_space=pltpu.SMEM)
    moved = (
        tokens,
        attn_gain.reshape(1, cols),
        query_weight,
        key_weight,
        value_weight,
        forget_weight.T,
        cache_keys,
        cache_values,
        gate_sum,
        out_blocks,
        mlp_gain.reshape(1, width),
        up_weight,
        down_weight,
    )
    scratch = [
        vm((rows, cols), BF),
        vm((1, cols), F32),
        vm(query_weight.shape, BF),
        vm(key_weight.shape, BF),
        vm(value_weight.shape, BF),
        vm(forget_weight.shape[::-1], BF),
        vm(cache_keys.shape, BF),
        vm(cache_values.shape, BF),
        vm(gate_sum.shape, F32),
        vm((chunks, local, HD, cols), BF),
        vm((1, width), F32),
        vm(up_weight.shape, BF),
        vm(down_weight.shape, BF),
        vm((PAD, cols), F32),
        vm((PAD, q_cols + 2 * kv_cols), F32),
        vm((PAD, q_cols + 2 * kv_cols), BF),
        vm((peers, PAD, q_cols + 2 * kv_cols), BF),
        vm((PAD, LANES), F32),
        vm((peers, PAD, LANES), F32),
        vm((chunks, PAD, LANES), F32),
        vm((rows * chunks, LANES), BF),
        vm((peers, rows * chunks, LANES), BF),
        vm((chunks, LANES), F32),
        vm((peers, chunks, LANES), F32),
        vm((chunks, PAD, LANES), F32),
        vm((kv_n, tp_n, PAD, cols), BF),
        vm((PAD, width), F32),
        vm((PAD, units), BF),
        vm((n, PAD, out_cols), BF),
        vm((n, PAD, out_cols), BF),
        dma((11 + pieces,)),
        dma((up_tiles,)),
        dma((n,)),
    ]
    for count in ((pieces, peers), (peers,), (peers,), (peers,), (n,), (n,)):
        scratch += [dma(count), dma(count)]
    return pl.pallas_call(
        functools.partial(layer_kernel, kv_n, tp_n),
        out_shape=jax.ShapeDtypeStruct((rows, out_cols), BF),
        in_specs=[smem_spec] * 2 + [any_spec] * len(moved),
        out_specs=pl.BlockSpec(memory_space=pltpu.VMEM),
        scratch_shapes=scratch,
        compiler_params=pltpu.CompilerParams(
            collective_id=0, has_side_effects=True, vmem_limit_bytes=60 * 1024 * 1024
        ),
        name="layer",
    )(lengths, forget_offset, *moved)


def fits(kv_n, tp_n, tokens, query_weight, key_weight, forget_weight, up_weight, down_weight):
    rows, cols = tokens.shape
    held = 4 * query_weight.size + up_weight.size * 2 + down_weight.size * 2
    return (
        rows <= PAD
        and kv_n > 1
        and cols % LANES == 0
        and key_weight.shape[1] == LANES
        and HD * 2 == LANES
        and up_weight.shape[1] % (4 * LANES) == 0
        and down_weight.shape[1] % (kv_n * tp_n * LANES) == 0
        and held < 48 * 1024 * 1024
    )


def shards(*args):
    kv_n = lax.axis_size("kv")
    tp_n = lax.axis_size("tp")
    if fits(kv_n, tp_n, args[0], args[3], args[4], args[6], args[13], args[14]):
        return kernel_shards(kv_n, tp_n, *args)
    return general_shards(*args)


def solution(mesh):
    placed = (
        P("dp", "kv"),
        P("dp"),
        P("kv"),
        P("kv", "tp"),
        P("kv", "tp"),
        P("kv", "tp"),
        P(),
        P("tp"),
        P("dp", "kv", "tp"),
        P("dp", "kv", "tp"),
        P("dp", "tp", "kv"),
        P("tp", "kv"),
        P(),
        P(None, ("kv", "tp")),
        P(("kv", "tp"), None),
    )
    return jax.shard_map(
        shards, mesh=mesh, in_specs=placed, out_specs=P("dp", ("kv", "tp")), check_vma=False
    )
```
